32 devices in a mesh: grp: 2 (over y), sp: 4 (over z), tp: 4 (over x, core).
Axes of the slice: x: 2, y: 2, z: 4, core: 2. Of those that a mesh axis runs over, the one named last changes fastest.
Arguments:
- tokens: bfloat16 [3072, 2048], P(('grp', 'sp'), 'tp'), parts along dimension 0, may hold values from -15 to 15
- gate_weight: bfloat16 [2, 2048, 2048], P(None, 'sp', 'tp'), may hold values from -0.125 to 0.125
- inner_weight: bfloat16 [2, 2048, 2048], P(None, 'sp', 'tp'), may hold values from -0.125 to 0.125
- value_weight: bfloat16 [2, 2048, 2048], P(None, 'sp', 'tp'), may hold values from -0.125 to 0.125
- out_weight: bfloat16 [2, 2048, 2048], P(None, 'tp', 'sp'), may hold values from -0.125 to 0.125
- taps: bfloat16 [2, 3, 2048], P(None, None, 'tp'), may hold values from -3 to 3
- norm_gain: float32 [2, 2048], P(None, 'tp'), may hold values from 0.1 to 1.9
- norm_bias: float32 [2, 2048], P(None, 'tp'), may hold values from -1.5 to 1.5
Outputs:
- mixed: bfloat16 [3072, 2048], P(('grp', 'sp'), 'tp'), parts along dimension 0
The draws below stay inside these ranges and needn't reach their ends.
There are 2 independent parts, one for each index of `grp`. The reference program is written for one: setup_inputs(seed, part) draws one part's arguments, and reference() takes and returns one part's arrays. A program takes and returns all parts, laid end to end along the dimension named above; an argument that names none is the same for every part. Nothing has to cross between parts.
All inputs are finite; a program needn't handle non-finite values.
Results may differ from the reference program's by a relative error of at most 0.03.
Values may be sent and summed in bfloat16 or wider, within the bound.
A program may use at most 64 MiB of HBM per device.

```python
import jax
import jax.numpy as jnp
from jax import lax

D = 2048
LAYERS = 2
TOKENS = 1536
N_TP = 4


def draw_tokens(key, part):
    base_key = jax.random.fold_in(key, 11)
    scale_key = jax.random.fold_in(key, 12)
    base = jnp.clip(jax.random.normal(base_key, (TOKENS, D), jnp.float32), -6.0, 6.0)
    levels = jnp.exp(jax.random.uniform(scale_key, (D // 32,), jnp.float32, -0.9, 0.9))
    scales = jnp.repeat(levels, 32)
    return (base * scales[None, :]).astype(jnp.bfloat16)


def steps_of(key, shape, pieces, least, high):
    factor_of = 1.0
    for axis_at, shards_of in pieces:
        steps = jax.random.uniform(jax.random.fold_in(jax.random.fold_in(key, 6), axis_at), (shards_of,), jnp.float32, least / len(pieces), high / len(pieces))
        factor_of = factor_of * jnp.repeat(jnp.exp(steps), shape[axis_at] // shards_of).reshape((-1,) + (1,) * (len(shape) - 1 - axis_at))
    return factor_of


def scatter_about(own_key, dims, scale, most, split=(), kind=jnp.bfloat16):
    drawn = jax.random.normal(own_key, dims, jnp.float32) * scale
    if len(split) > 0:
        drawn = steps_of(own_key, dims, split, -0.22, 0.18) * drawn
    return jnp.clip(drawn, min=-most, max=most).astype(kind)


def setup_inputs(seed: int = 0, part: int = 0) -> dict:
    key_of = jax.random.split(jax.random.key(seed), 9)
    part_splits = jax.random.split(jax.random.fold_in(key_of[8], part), 9)
    return {
        "tokens": draw_tokens(jax.random.fold_in(jax.random.fold_in(key_of[8], part), 71), part),
        "gate_weight": scatter_about(key_of[1], (LAYERS, D, D), D ** -0.5, 0.125, ((1, 4), (2, 4))),
        "inner_weight": scatter_about(key_of[2], (LAYERS, D, D), D ** -0.5, 0.125, ((1, 4), (2, 4))),
        "value_weight": scatter_about(key_of[3], (LAYERS, D, D), D ** -0.5, 0.125, ((1, 4), (2, 4))),
        "out_weight": scatter_about(key_of[4], (LAYERS, D, D), D ** -0.5, 0.125, ((1, 4), (2, 4))),
        "taps": scatter_about(key_of[5], (LAYERS, 3, D), 0.6, 3.0, ((2, 4),)),
        "norm_gain": jnp.clip(1.0 + 0.18 * jax.random.normal(key_of[6], (LAYERS, D), jnp.float32), 0.1, 1.9),
        "norm_bias": scatter_about(key_of[7], (LAYERS, D), 0.3, 1.5, ((1, 4),), jnp.float32),
    }


def reference(tokens, gate_weight, inner_weight, value_weight, out_weight, taps, norm_gain, norm_bias):
    x = tokens
    block = D // N_TP
    for layer in range(LAYERS):
        outer = jnp.dot(x, gate_weight[layer], preferred_element_type=jnp.float32).astype(jnp.bfloat16)
        inner = jnp.dot(x, inner_weight[layer], preferred_element_type=jnp.float32).astype(jnp.bfloat16)
        values = jnp.dot(x, value_weight[layer], preferred_element_type=jnp.float32).astype(jnp.bfloat16)
        product = (inner.astype(jnp.float32) * values.astype(jnp.float32)).astype(jnp.bfloat16)
        padded = jnp.pad(product.astype(jnp.float32), ((1, 1), (0, 0)))
        kernel = taps[layer].astype(jnp.float32)
        conv = kernel[0] * padded[:-2] + kernel[1] * padded[1:-1] + kernel[2] * padded[2:]
        gated = (outer.astype(jnp.float32) * conv).astype(jnp.bfloat16)
        branch = jnp.zeros((x.shape[0], D), jnp.float32)
        for index in range(N_TP):
            part_rows = gated[:, index * block:(index + 1) * block]
            part_weight = out_weight[layer][index * block:(index + 1) * block, :]
            term = jnp.dot(part_rows, part_weight, preferred_element_type=jnp.float32).astype(jnp.bfloat16)
            branch = branch + term.astype(jnp.float32)
        total = 2.0 ** 0.5 * x.astype(jnp.float32) + branch
        mean = lax.optimization_barrier(jnp.sum(total, axis=1, keepdims=True)) / D
        square = lax.optimization_barrier(jnp.sum(total * total, axis=1, keepdims=True)) / D
        spread = square - mean * mean
        x = ((total - mean) * lax.rsqrt(spread + 1e-05) * norm_gain[layer] + norm_bias[layer]).astype(jnp.bfloat16)
    return x
```

```python
import functools

import jax
import jax.numpy as jnp
from jax import lax
from jax.experimental import pallas as pl
from jax.experimental.pallas import tpu as pltpu
from jax.sharding import PartitionSpec as P

MESH = pl.DeviceIdType.MESH
F32 = jnp.float32
BF16 = jnp.bfloat16


def extended(value, sides, width):
    for axis, dim in sides:
        peers, length = (lax.axis_size(axis), value.shape[dim])
        up = [(i, (i + 1) % peers) for i in range(peers - 1)]
        down = [(j, i) for i, j in up]
        last = lax.slice_in_dim(value, length - width, length, axis=dim)
        initial = lax.slice_in_dim(value, 0, width, axis=dim)
        before = lax.ppermute(last, axis, up)
        after = lax.ppermute(initial, axis, down)
        value = jnp.concatenate([before, value, after], axis=dim)
    return value


def shards(tokens, gate_weight, inner_weight, value_weight, out_weight, taps, norm_gain, norm_bias):
    x = tokens
    width = x.shape[1] * lax.axis_size("tp")
    full_gate, full_inner, full_value, full_out = (
        lax.all_gather(gate_weight, "sp", axis=1, tiled=True),
        lax.all_gather(inner_weight, "sp", axis=1, tiled=True),
        lax.all_gather(value_weight, "sp", axis=1, tiled=True),
        lax.all_gather(out_weight, "sp", axis=2, tiled=True),
    )
    for layer in range(gate_weight.shape[0]):
        whole = lax.all_gather(x, "tp", axis=1, tiled=True)
        outer = jnp.dot(whole, full_gate[layer], preferred_element_type=F32).astype(BF16)
        inner = jnp.dot(whole, full_inner[layer], preferred_element_type=F32).astype(BF16)
        values = jnp.dot(whole, full_value[layer], preferred_element_type=F32).astype(BF16)
        product = (inner.astype(F32) * values.astype(F32)).astype(BF16)
        padded = extended(product, (("sp", 0),), 1).astype(F32)
        kernel = taps[layer].astype(F32)
        conv = kernel[0] * padded[:-2] + kernel[1] * padded[1:-1] + kernel[2] * padded[2:]
        gated = (outer.astype(F32) * conv).astype(BF16)
        terms = jnp.dot(gated, full_out[layer], preferred_element_type=F32)
        branch = lax.psum_scatter(
            terms.astype(BF16), "tp", scatter_dimension=1, tiled=True
        ).astype(F32)
        total = 2.0**0.5 * x.astype(F32) + branch
        row_sum, row_square = lax.psum(
            (jnp.sum(total, axis=1), jnp.sum(total * total, axis=1)), "tp"
        )
        mean = (row_sum / width)[:, None]
        spread = (row_square / width)[:, None] - mean * mean
        x = (
            (total - mean) * lax.rsqrt(spread + 1e-05) * norm_gain[layer] + norm_bias[layer]
        ).astype(BF16)
    return x


def mixer(layers, x_hbm, wi, wv, wg, wo, taps, gain, bias, out,
          gbuf, xfull, ibuf, pbuf, obuf, gated, tot, halo,
          sib_out, sib_in, far_out, far_in, st_out, st_in,
          s_local, s_x, s_own_r, s_own_l, s_fwd, s_y, r_z, r_y,
          s_halo, r_halo, s_ag, r_ag, s_rs, r_rs, s_st, r_st):
    g, s, t = lax.axis_index("grp"), lax.axis_index("sp"), lax.axis_index("tp")
    weights = (wi, wv, wg, wo)
    rows, chan = x_hbm.shape
    block = chan
    half = block // 2
    width = xfull.shape[2]
    units = 4 * layers
    last = lax.axis_size("sp") - 1
    sib = t + 1 - 2 * lax.rem(t, 2)
    far = lax.rem(t + 2, 4)
    diag = lax.rem(sib + 2, 4)
    own = pl.ds(pl.multiple_of(t * chan, 128), chan)
    grp_peer = 1 - g

    def local(u):
        layer, m = divmod(u, 4)
        return pltpu.make_async_copy(
            weights[m].at[layer],
            gbuf.at[u, pl.ds(pl.multiple_of(s * block, block), block)],
            s_local.at[u])

    x_copy = pltpu.make_async_copy(x_hbm, xfull.at[0, :, own], s_x)
    x_copy.start()
    for u in range(units):
        local(u).start()

    barrier = pltpu.get_barrier_semaphore()

    def hello(dg, ds, dt):
        pl.semaphore_signal(barrier, 1, device_id=(dg, ds, dt), device_id_type=MESH)

    hello(grp_peer, s, t)
    for k in (1, 2, 3):
        hello(g, s, lax.rem(t + k, 4))

    @pl.when(s > 0)
    def _():
        hello(g, s - 1, t)

    @pl.when(s < last)
    def _():
        hello(g, s + 1, t)

    pl.semaphore_wait(barrier, 4 + jnp.where(s > 0, 1, 0) + jnp.where(s < last, 1, 0))

    def piece(u, src, side):
        return gbuf.at[u, pl.ds(pl.multiple_of(src * block + side * half, half), half)]

    def remote(src, dst, send, recv, to):
        return pltpu.make_async_remote_copy(
            src_ref=src, dst_ref=dst, send_sem=send, recv_sem=recv,
            device_id=to, device_id_type=MESH)

    def own_right(u):
        p = piece(u, s, g)
        return remote(p, p, s_own_r.at[u], r_z.at[u, s], (g, s + 1, t))

    def own_left(u):
        p = piece(u, s, g)
        return remote(p, p, s_own_l.at[u], r_z.at[u, s], (g, s - 1, t))

    sources = (
        s + 1 - 2 * lax.rem(s, 2),
        jnp.where(s < 2, 2, 1),
        jnp.where(s < 2, 3, 0),
    )

    def forward(u, k):
        src = sources[k]
        p = piece(u, src, g)
        return remote(p, p, s_fwd.at[u, k], r_z.at[u, src],
                      (g, jnp.where(src > s, s - 1, s + 1), t))

    def across(u, k, side):
        src = sources[k]
        p = piece(u, src, side)
        return remote(p, p, s_y.at[u, k], r_y.at[u, k], (grp_peer, s, t))

    middle = jnp.logical_and(s > 0, s < last)

    def send_own(u):
        local(u).wait()

        @pl.when(s < last)
        def _():
            own_right(u).start()

        @pl.when(s > 0)
        def _():
            own_left(u).start()

    def event(u, k):
        src = sources[k]
        p = piece(u, src, g)
        remote(p, p, s_fwd.at[u, k], r_z.at[u, src], (grp_peer, s, t)).wait_recv()

        @pl.when(middle)
        def _():
            forward(u, k).start()

        across(u, k, g).start()

    def unit_ready(u):
        for k in range(3):
            across(u, k, grp_peer).wait_recv()

    def column(owner):
        return pl.ds(pl.multiple_of(owner * chan, 128), chan)

    def ag(layer, i):
        owner = (t, t, far)[i]
        to = (far, sib, sib)[i]
        ref = xfull.at[layer, :, column(owner)]
        return remote(ref, ref, s_ag.at[layer, i], r_ag.at[layer, i], (g, s, to))

    def ag_recv(layer, i):
        owner = (far, sib, diag)[i]
        ref = xfull.at[layer, :, column(owner)]
        remote(ref, ref, s_ag.at[layer, i], r_ag.at[layer, i], (g, s, sib)).wait_recv()

    def ag_start(layer):
        ag(layer, 0).start()
        ag(layer, 1).start()

    def ag_forward(layer):
        ag_recv(layer, 0)
        ag(layer, 2).start()

    def ag_finish(layer):
        ag_recv(layer, 1)
        ag_recv(layer, 2)

    tile = 256

    def project(layer, m, store):
        u = 4 * layer + m
        unit_ready(u)

        @pl.loop(0, chan // tile)
        def _(n):
            cols = pl.ds(pl.multiple_of(n * tile, tile), tile)
            store(cols, jnp.dot(xfull[layer], gbuf[u, :, cols],
                                preferred_element_type=F32).astype(BF16))

    edge = halo.shape[2]

    def halo_up(layer):
        return remote(pbuf.at[layer, pl.ds(rows - edge, edge)], halo.at[layer, 0],
                      s_halo.at[layer, 0], r_halo.at[layer, 0], (g, s + 1, t))

    def halo_down(layer):
        return remote(pbuf.at[layer, pl.ds(0, edge)], halo.at[layer, 1],
                      s_halo.at[layer, 1], r_halo.at[layer, 1], (g, s - 1, t))

    def do_inner(layer):
        def store(cols, value):
            ibuf[:, cols] = value
        project(layer, 0, store)

    def do_value(layer):
        def store(cols, value):
            pbuf[layer, :, cols] = (ibuf[:, cols].astype(F32) * value.astype(F32)).astype(BF16)
        project(layer, 1, store)

        @pl.when(s < last)
        def _():
            halo_up(layer).start()

        @pl.when(s > 0)
        def _():
            halo_down(layer).start()

    def do_gate(layer):
        def store(cols, value):
            obuf[:, cols] = value
        project(layer, 2, store)

    def do_conv(layer):
        @pl.when(s > 0)
        def _():
            halo_up(layer).wait_recv()

        @pl.when(s < last)
        def _():
            halo_down(layer).wait_recv()

        @pl.loop(0, chan // 128)
        def _(n):
            cols = pl.ds(pl.multiple_of(n * 128, 128), 128)
            p = pbuf[layer, :, cols].astype(F32)
            row = lax.broadcasted_iota(jnp.int32, p.shape, 0)
            first = jnp.where(s > 0, halo[layer, 0, :, cols].astype(F32)[edge - 1:edge], 0.0)
            final = jnp.where(s < last, halo[layer, 1, :, cols].astype(F32)[0:1], 0.0)
            before = jnp.where(row == 0, first, pltpu.roll(p, 1, 0))
            after = jnp.where(row == rows - 1, final, pltpu.roll(p, rows - 1, 0))
            k = taps[layer, :, cols].astype(F32)
            conv = k[0:1] * before + k[1:2] * p + k[2:3] * after
            gated[:, cols] = (obuf[:, cols].astype(F32) * conv).astype(BF16)

    def term(layer, owner, store):
        u = 4 * layer + 3

        @pl.loop(0, chan // tile)
        def _(n):
            cols = pl.ds(pl.multiple_of(n * tile, tile), tile)
            w = gbuf[u, pl.ds(pl.multiple_of(owner * block, block), block), cols]
            store(cols, jnp.dot(gated[...], w, preferred_element_type=F32).astype(BF16))

    def to_sib(layer, i):
        return remote(sib_out.at[layer, i], sib_in.at[layer, i],
                      s_rs.at[layer, i], r_rs.at[layer, i], (g, s, sib))

    def to_far(layer):
        return remote(far_out.at[layer], far_in.at[layer],
                      s_rs.at[layer, 2], r_rs.at[layer, 2], (g, s, far))

    def do_out(layer):
        unit_ready(4 * layer + 3)
        for i, owner in ((0, diag), (1, sib)):
            def store(cols, value):
                sib_out[layer, i, :, cols] = value
            term(layer, owner, store)
            to_sib(layer, i).start()

    def do_far(layer):
        to_sib(layer, 0).wait_recv()

        def store(cols, value):
            far_out[layer, :, cols] = (
                value.astype(F32) + sib_in[layer, 0, :, cols].astype(F32)).astype(BF16)
        term(layer, far, store)
        to_far(layer).start()

    def stat(layer, i):
        return remote(st_out.at[layer], st_in.at[layer, i], s_st.at[layer, i],
                      r_st.at[layer, i], (g, s, (sib, far, diag)[i]))

    def do_total(layer):
        to_sib(layer, 1).wait_recv()

        def store(cols, value):
            mine = pl.ds(pl.multiple_of(t * chan + cols.start, 128), tile)
            tot[:, cols] = (2.0**0.5 * xfull[layer, :, mine].astype(F32) + value.astype(F32)
                            + sib_in[layer, 1, :, cols].astype(F32))
        term(layer, t, store)

    def do_stats(layer):
        to_far(layer).wait_recv()
        total_sum = jnp.zeros((rows, 128), F32)
        total_square = jnp.zeros((rows, 128), F32)
        for n in range(chan // 128):
            cols = slice(n * 128, n * 128 + 128)
            z = tot[:, cols] + far_in[layer, :, cols].astype(F32)
            tot[:, cols] = z
            total_sum = total_sum + z
            total_square = total_square + z * z
        st_out[layer, 0:1, :] = jnp.sum(total_sum.T, axis=0, keepdims=True)
        st_out[layer, 1:2, :] = jnp.sum(total_square.T, axis=0, keepdims=True)
        for i in range(3):
            stat(layer, i).start()

    def do_norm(layer, store):
        for i in range(3):
            stat(layer, i).wait_recv()
        both = st_out[layer] + st_in[layer, 0] + st_in[layer, 1] + st_in[layer, 2]
        mean = both[0:1] / width
        spread = both[1:2] / width - mean * mean
        scale = lax.rsqrt(spread + 1e-05)
        mean = jnp.broadcast_to(mean, (128, rows)).T
        scale = jnp.broadcast_to(scale, (128, rows)).T
        for n in range(chan // 128):
            cols = slice(n * 128, n * 128 + 128)
            z = (tot[:, cols] - mean) * scale * gain[layer:layer + 1, cols] + bias[layer:layer + 1, cols]
            store(n, z.astype(BF16))

    def do_next(layer):
        def store(n, value):
            xfull[layer + 1, :, pl.ds(pl.multiple_of(t * chan + n * 128, 128), 128)] = value
        do_norm(layer, store)
        ag_start(layer + 1)

    def do_result(layer):
        def store(n, value):
            out[:, n * 128:n * 128 + 128] = value
        do_norm(layer, store)

    st_out[...] = jnp.zeros_like(st_out)
    ahead = 2
    for u in range(min(ahead, units)):
        send_own(u)
    x_copy.wait()
    ag_start(0)

    steps = {}

    def put(u, k, step, layer):
        at = min(3 * u + k, 3 * units - 1)
        steps.setdefault(at, []).append((step, layer))

    put(0, 1, ag_forward, 0)
    put(0, 2, ag_finish, 0)
    for layer in range(layers):
        b = 4 * layer
        if layer > 0:
            put(b + 2, 1, ag_forward, layer)
            put(b + 2, 2, ag_finish, layer)
            put(b + 2, 2, do_inner, layer)
            put(b + 3, 0, do_value, layer)
            put(b + 3, 1, do_gate, layer)
        else:
            put(b + 1, 1, do_inner, layer)
            put(b + 2, 1, do_value, layer)
            put(b + 3, 1, do_gate, layer)
        put(b + 3, 2, do_conv, layer)
        put(b + 4, 1, do_out, layer)
        put(b + 4, 2, do_far, layer)
        put(b + 4, 2, do_total, layer)
        put(b + 5, 1, do_stats, layer)
        put(b + 5, 2, do_next if layer < layers - 1 else do_result, layer)

    for u in range(units):
        if u + ahead < units:
            send_own(u + ahead)
        for k in range(3):
            event(u, k)
            for step, layer in steps.get(3 * u + k, ()):
                step(layer)

    for u in range(units):
        @pl.when(s < last)
        def _():
            own_right(u).wait_send()

        @pl.when(s > 0)
        def _():
            own_left(u).wait_send()

        for k in range(3):
            @pl.when(middle)
            def _():
                forward(u, k).wait_send()

            across(u, k, g).wait_send()
    for layer in range(layers):
        @pl.when(s < last)
        def _():
            halo_up(layer).wait_send()

        @pl.when(s > 0)
        def _():
            halo_down(layer).wait_send()

        for i in range(3):
            ag(layer, i).wait_send()
            stat(layer, i).wait_send()
        to_sib(layer, 0).wait_send()
        to_sib(layer, 1).wait_send()
        to_far(layer).wait_send()


def fused(tokens, gate_weight, inner_weight, value_weight, out_weight, taps, norm_gain, norm_bias):
    rows, chan = tokens.shape
    layers = gate_weight.shape[0]
    width = chan * lax.axis_size("tp")
    units = 4 * layers
    dma = pltpu.SemaphoreType.DMA
    hbm = pl.BlockSpec(memory_space=pltpu.HBM)
    vmem = pl.BlockSpec(memory_space=pltpu.VMEM)
    return pl.pallas_call(
        functools.partial(mixer, layers),
        out_shape=jax.ShapeDtypeStruct((rows, chan), BF16),
        in_specs=[hbm] * 5 + [vmem] * 3,
        out_specs=vmem,
        scratch_shapes=[
            pltpu.VMEM((units, width, chan), BF16),
            pltpu.VMEM((layers, rows, width), BF16),
            pltpu.VMEM((rows, chan), BF16),
            pltpu.VMEM((layers, rows, chan), BF16),
            pltpu.VMEM((rows, chan), BF16),
            pltpu.VMEM((rows, chan), BF16),
            pltpu.VMEM((rows, chan), F32),
            pltpu.VMEM((layers, 2, 16, chan), BF16),
            pltpu.VMEM((layers, 2, rows, chan), BF16),
            pltpu.VMEM((layers, 2, rows, chan), BF16),
            pltpu.VMEM((layers, rows, chan), BF16),
            pltpu.VMEM((layers, rows, chan), BF16),
            pltpu.VMEM((layers, 8, rows), F32),
            pltpu.VMEM((layers, 3, 8, rows), F32),
            dma((units,)), dma, dma((units,)), dma((units,)),
            dma((units, 3)), dma((units, 3)), dma((units, 4)), dma((units, 3)),
            dma((layers, 2)), dma((layers, 2)), dma((layers, 3)), dma((layers, 3)),
            dma((layers, 3)), dma((layers, 3)), dma((layers, 3)), dma((layers, 3)),
        ],
        compiler_params=pltpu.CompilerParams(
            collective_id=0, has_side_effects=True, vmem_limit_bytes=48 * 2**20),
    )(tokens, inner_weight, value_weight, gate_weight, out_weight, taps, norm_gain, norm_bias)


def solution(mesh):
    in_specs = (
        P(("grp", "sp"), "tp"),
        P(None, "sp", "tp"),
        P(None, "sp", "tp"),
        P(None, "sp", "tp"),
        P(None, "tp", "sp"),
        P(None, None, "tp"),
        P(None, "tp"),
        P(None, "tp"),
    )
    out_specs = P(("grp", "sp"), "tp")
    routed = (mesh.shape["grp"], mesh.shape["sp"], mesh.shape["tp"]) == (2, 4, 4)
    body = fused if routed else shards
    return jax.shard_map(body, mesh=mesh, in_specs=in_specs, out_specs=out_specs, check_vma=False)
```

```python
import functools

import jax
import jax.numpy as jnp
from jax import lax
from jax.experimental import pallas as pl
from jax.experimental.pallas import tpu as pltpu
from jax.sharding import PartitionSpec as P

MESH = pl.DeviceIdType.MESH
F32 = jnp.float32
BF16 = jnp.bfloat16


def extended(value, sides, width):
    for axis, dim in sides:
        peers, length = (lax.axis_size(axis), value.shape[dim])
        up = [(i, (i + 1) % peers) for i in range(peers - 1)]
        down = [(j, i) for i, j in up]
        last = lax.slice_in_dim(value, length - width, length, axis=dim)
        initial = lax.slice_in_dim(value, 0, width, axis=dim)
        before = lax.ppermute(last, axis, up)
        after = lax.ppermute(initial, axis, down)
        value = jnp.concatenate([before, value, after], axis=dim)
    return value


def shards(tokens, gate_weight, inner_weight, value_weight, out_weight, taps, norm_gain, norm_bias):
    x = tokens
    width = x.shape[1] * lax.axis_size("tp")
    full_gate, full_inner, full_value, full_out = (
        lax.all_gather(gate_weight, "sp", axis=1, tiled=True),
        lax.all_gather(inner_weight, "sp", axis=1, tiled=True),
        lax.all_gather(value_weight, "sp", axis=1, tiled=True),
        lax.all_gather(out_weight, "sp", axis=2, tiled=True),
    )
    for layer in range(gate_weight.shape[0]):
        whole = lax.all_gather(x, "tp", axis=1, tiled=True)
        outer = jnp.dot(whole, full_gate[layer], preferred_element_type=F32).astype(BF16)
        inner = jnp.dot(whole, full_inner[layer], preferred_element_type=F32).astype(BF16)
        values = jnp.dot(whole, full_value[layer], preferred_element_type=F32).astype(BF16)
        product = (inner.astype(F32) * values.astype(F32)).astype(BF16)
        padded = extended(product, (("sp", 0),), 1).astype(F32)
        kernel = taps[layer].astype(F32)
        conv = kernel[0] * padded[:-2] + kernel[1] * padded[1:-1] + kernel[2] * padded[2:]
        gated = (outer.astype(F32) * conv).astype(BF16)
        terms = jnp.dot(gated, full_out[layer], preferred_element_type=F32)
        branch = lax.psum_scatter(
            terms.astype(BF16), "tp", scatter_dimension=1, tiled=True
        ).astype(F32)
        total = 2.0**0.5 * x.astype(F32) + branch
        row_sum, row_square = lax.psum(
            (jnp.sum(total, axis=1), jnp.sum(total * total, axis=1)), "tp"
        )
        mean = (row_sum / width)[:, None]
        spread = (row_square / width)[:, None] - mean * mean
        x = (
            (total - mean) * lax.rsqrt(spread + 1e-05) * norm_gain[layer] + norm_bias[layer]
        ).astype(BF16)
    return x


def mixer(layers, x_hbm, wi, wv, wg, wo, taps, gain, bias, out,
          gbuf, xfull, ibuf, pbuf, obuf, gated, tot, halo, final,
          sib_out, sib_in, far_out, far_in, st_out, st_in,
          s_local, s_x, s_own, s_fwd, s_y, r_z, r_y,
          s_end, r_end, s_tok, r_tok, s_res, r_res,
          s_halo, r_halo, s_ag, r_ag, s_rs, r_rs, s_st, r_st):
    g, s, t = lax.axis_index("grp"), lax.axis_index("sp"), lax.axis_index("tp")
    weights = (wi, wv, wg, wo)
    rows, chan = x_hbm.shape
    block = chan
    half = block // 2
    width = xfull.shape[2]
    units = 4 * layers
    last = lax.axis_size("sp") - 1
    sib = t + 1 - 2 * lax.rem(t, 2)
    far = lax.rem(t + 2, 4)
    diag = lax.rem(sib + 2, 4)
    grp_peer = 1 - g
    is_end = jnp.logical_or(s == 0, s == last)
    is_middle = jnp.logical_and(s > 0, s < last)
    mate = s + 1 - 2 * lax.rem(s, 2)
    inner = last - s
    beyond = last - mate

    def column(owner):
        return pl.ds(pl.multiple_of(owner * chan, 128), chan)

    def token_rows(h):
        holder = mate if h == 0 else s
        return pl.ds(pl.multiple_of(lax.rem(holder, 2) * rows, rows), rows)

    def local(u):
        layer, m = divmod(u, 4)
        return pltpu.make_async_copy(
            weights[m].at[layer],
            gbuf.at[u, pl.ds(pl.multiple_of(s * block, block), block)],
            s_local.at[u])

    x_copy = pltpu.make_async_copy(x_hbm, xfull.at[0, token_rows(1), column(t)], s_x)
    x_copy.start()
    for u in range(units):
        local(u).start()

    barrier = pltpu.get_barrier_semaphore()

    def hello(dg, ds, dt):
        pl.semaphore_signal(barrier, 1, device_id=(dg, ds, dt), device_id_type=MESH)

    hello(g, mate, t)

    @pl.when(is_middle)
    def _():
        hello(grp_peer, s, t)
        hello(g, inner, t)
        for k in (1, 2, 3):
            hello(g, s, lax.rem(t + k, 4))

    pl.semaphore_wait(barrier, jnp.where(is_middle, 6, 1))

    def remote(src, dst, send, recv, to):
        return pltpu.make_async_remote_copy(
            src_ref=src, dst_ref=dst, send_sem=send, recv_sem=recv,
            device_id=to, device_id_type=MESH)

    def piece(u, src, side):
        return gbuf.at[u, pl.ds(pl.multiple_of(src * block + side * half, half), half)]

    def tokens_in():
        ref = xfull.at[0, token_rows(1), column(t)]
        return remote(ref, ref, s_tok, r_tok, (g, mate, t))

    def end_piece(u, i):
        p = piece(u, s, g if i == 0 else 1 - g)
        return remote(p, p, s_end.at[u, i], r_end.at[u, i], (g, mate, t))

    def result():
        return remote(final, out, s_res, r_res, (g, mate, t))

    @pl.when(is_end)
    def _():
        x_copy.wait()
        tokens_in().start()
        for u in range(units):
            local(u).wait()
            if u >= 2:
                end_piece(u - 2, 0).wait_send()
                end_piece(u - 2, 1).wait_send()
            end_piece(u, 0).start()
            end_piece(u, 1).start()
        for u in range(units - 2, units):
            end_piece(u, 0).wait_send()
            end_piece(u, 1).wait_send()
        tokens_in().wait_send()
        result().wait_recv()

    def own_in(u):
        p = piece(u, s, g)
        return remote(p, p, s_own.at[u], r_z.at[u, 0], (g, inner, t))

    def forward(u):
        p = piece(u, mate, g)
        return remote(p, p, s_fwd.at[u], r_z.at[u, 1], (g, inner, t))

    def across(u, k, side):
        p = piece(u, inner if k == 0 else beyond, side)
        return remote(p, p, s_y.at[u, k], r_y.at[u, k], (grp_peer, s, t))

    def event(u, k):
        if k == 0:
            p = piece(u, mate, g)
            remote(p, p, s_end.at[u, 0], r_end.at[u, 0], (g, mate, t)).wait_recv()
            forward(u).start()
        else:
            p = piece(u, inner if k == 1 else beyond, g)
            remote(p, p, s_fwd.at[u], r_z.at[u, k - 1], (g, inner, t)).wait_recv()
            across(u, k - 1, g).start()

    def send_own(u):
        local(u).wait()
        own_in(u).start()

    def unit_ready(u):
        p = piece(u, mate, 1 - g)
        remote(p, p, s_end.at[u, 1], r_end.at[u, 1], (g, mate, t)).wait_recv()
        across(u, 0, grp_peer).wait_recv()
        across(u, 1, grp_peer).wait_recv()

    def ag(layer, h, i):
        owner = (t, t, far)[i]
        to = (far, sib, sib)[i]
        ref = xfull.at[layer, token_rows(h), column(owner)]
        return remote(ref, ref, s_ag.at[layer, h, i], r_ag.at[layer, h, i], (g, s, to))

    def ag_recv(layer, h, i):
        owner = (far, sib, diag)[i]
        ref = xfull.at[layer, token_rows(h), column(owner)]
        remote(ref, ref, s_ag.at[layer, h, i], r_ag.at[layer, h, i], (g, s, sib)).wait_recv()

    def ag_start(layer, h):
        ag(layer, h, 0).start()
        ag(layer, h, 1).start()

    def ag_forward(layer, h):
        ag_recv(layer, h, 0)
        ag(layer, h, 2).start()

    def ag_finish(layer, h):
        ag_recv(layer, h, 1)
        ag_recv(layer, h, 2)

    def adopt():
        ref = xfull.at[0, token_rows(0), column(t)]
        remote(ref, ref, s_tok, r_tok, (g, mate, t)).wait_recv()
        ag_start(0, 0)

    tile = 256
    tiles = chan // tile

    def project(layer, m, store):
        u = 4 * layer + m
        unit_ready(u)

        @pl.loop(0, 2 * tiles)
        def _(n):
            cols = pl.ds(pl.multiple_of(lax.rem(n, tiles) * tile, tile), tile)
            at = pl.ds(pl.multiple_of((n // tiles) * rows, rows), rows)
            store(at, cols, jnp.dot(xfull[layer, at, :], gbuf[u, :, cols],
                                    preferred_element_type=F32).astype(BF16))

    edge = halo.shape[1]

    def halo_copy(layer):
        edge_row = jnp.where(s < inner, 2 * rows - edge, 0)
        return remote(pbuf.at[layer, pl.ds(pl.multiple_of(edge_row, edge), edge)], halo.at[layer],
                      s_halo.at[layer], r_halo.at[layer], (g, inner, t))

    def do_inner(layer):
        def store(at, cols, value):
            ibuf[at, cols] = value
        project(layer, 0, store)

    def do_value(layer):
        def store(at, cols, value):
            pbuf[layer, at, cols] = (ibuf[at, cols].astype(F32) * value.astype(F32)).astype(BF16)
        project(layer, 1, store)
        halo_copy(layer).start()

    def do_gate(layer):
        def store(at, cols, value):
            obuf[at, cols] = value
        project(layer, 2, store)

    def do_conv(layer):
        halo_copy(layer).wait_recv()

        @pl.loop(0, chan // 128)
        def _(n):
            cols = pl.ds(pl.multiple_of(n * 128, 128), 128)
            p = pbuf[layer, :, cols].astype(F32)
            row = lax.broadcasted_iota(jnp.int32, p.shape, 0)
            met = halo[layer, :, cols].astype(F32)
            first = jnp.where(s > inner, met[edge - 1:edge], 0.0)
            closing = jnp.where(s < inner, met[0:1], 0.0)
            before = jnp.where(row == 0, first, pltpu.roll(p, 1, 0))
            after = jnp.where(row == 2 * rows - 1, closing, pltpu.roll(p, 2 * rows - 1, 0))
            k = taps[layer, :, cols].astype(F32)
            conv = k[0:1] * before + k[1:2] * p + k[2:3] * after
            gated[:, cols] = (obuf[:, cols].astype(F32) * conv).astype(BF16)

    def term(layer, h, owner, store):
        u = 4 * layer + 3
        at = token_rows(h)

        @pl.loop(0, tiles)
        def _(n):
            cols = pl.ds(pl.multiple_of(n * tile, tile), tile)
            w = gbuf[u, pl.ds(pl.multiple_of(owner * block, block), block), cols]
            store(cols, jnp.dot(gated[at, :], w, preferred_element_type=F32).astype(BF16))

    def to_sib(layer, h, i):
        return remote(sib_out.at[layer, h, i], sib_in.at[layer, h, i],
                      s_rs.at[layer, h, i], r_rs.at[layer, h, i], (g, s, sib))

    def to_far(layer, h):
        return remote(far_out.at[layer, h], far_in.at[layer, h],
                      s_rs.at[layer, h, 2], r_rs.at[layer, h, 2], (g, s, far))

    def do_diag(layer, h):
        def store(cols, value):
            sib_out[layer, h, 0, :, cols] = value
        term(layer, h, diag, store)
        to_sib(layer, h, 0).start()

    def do_sib(layer, h):
        def store(cols, value):
            sib_out[layer, h, 1, :, cols] = value
        term(layer, h, sib, store)
        to_sib(layer, h, 1).start()

    def do_far(layer, h):
        to_sib(layer, h, 0).wait_recv()

        def store(cols, value):
            far_out[layer, h, :, cols] = (
                value.astype(F32) + sib_in[layer, h, 0, :, cols].astype(F32)).astype(BF16)
        term(layer, h, far, store)
        to_far(layer, h).start()

    def do_out(layer):
        unit_ready(4 * layer + 3)
        do_diag(layer, 0)
        do_diag(layer, 1)
        do_far(layer, 0)
        do_far(layer, 1)
        do_sib(layer, 0)
        do_sib(layer, 1)
        do_total(layer, 0)
        do_total(layer, 1)

    def stat(layer, h, i):
        return remote(st_out.at[layer, h], st_in.at[layer, h, i], s_st.at[layer, h, i],
                      r_st.at[layer, h, i], (g, s, (sib, far, diag)[i]))

    def do_total(layer, h):
        to_sib(layer, h, 1).wait_recv()
        at = token_rows(h)

        def store(cols, value):
            mine = pl.ds(pl.multiple_of(t * chan + cols.start, 128), tile)
            tot[h, :, cols] = (2.0**0.5 * xfull[layer, at, mine].astype(F32) + value.astype(F32)
                               + sib_in[layer, h, 1, :, cols].astype(F32))
        term(layer, h, t, store)

    def do_stats(layer, h):
        to_far(layer, h).wait_recv()
        total_sum = jnp.zeros((rows, 128), F32)
        total_square = jnp.zeros((rows, 128), F32)
        for n in range(chan // 128):
            cols = slice(n * 128, n * 128 + 128)
            z = tot[h, :, cols] + far_in[layer, h, :, cols].astype(F32)
            tot[h, :, cols] = z
            total_sum = total_sum + z
            total_square = total_square + z * z
        st_out[layer, h, 0:1, :] = jnp.sum(total_sum.T, axis=0, keepdims=True)
        st_out[layer, h, 1:2, :] = jnp.sum(total_square.T, axis=0, keepdims=True)
        for i in range(3):
            stat(layer, h, i).start()

    def do_norm(layer, h, store):
        for i in range(3):
            stat(layer, h, i).wait_recv()
        both = st_out[layer, h] + st_in[layer, h, 0] + st_in[layer, h, 1] + st_in[layer, h, 2]
        mean = both[0:1] / width
        spread = both[1:2] / width - mean * mean
        scale = lax.rsqrt(spread + 1e-05)
        mean = jnp.broadcast_to(mean, (128, rows)).T
        scale = jnp.broadcast_to(scale, (128, rows)).T
        for n in range(chan // 128):
            cols = slice(n * 128, n * 128 + 128)
            z = (tot[h, :, cols] - mean) * scale * gain[layer:layer + 1, cols] + bias[layer:layer + 1, cols]
            store(n, z.astype(BF16))

    def do_next(layer, h):
        at = token_rows(h)

        def store(n, value):
            xfull[layer + 1, at, pl.ds(pl.multiple_of(t * chan + n * 128, 128), 128)] = value
        do_norm(layer, h, store)
        ag_start(layer + 1, h)

    def do_result(layer, h):
        target = final if h == 0 else out

        def store(n, value):
            target[:, n * 128:n * 128 + 128] = value
        do_norm(layer, h, store)
        if h == 0:
            result().start()

    steps = {}

    def put(u, k, step, *args):
        at = min(3 * u + k, 3 * units - 1)
        steps.setdefault(at, []).append((step, args))

    put(0, 0, adopt)
    put(0, 1, ag_forward, 0, 1)
    put(1, 0, ag_forward, 0, 0)
    put(1, 0, ag_finish, 0, 1)
    put(1, 1, ag_finish, 0, 0)
    for layer in range(layers):
        b = 4 * layer
        if layer > 0:
            put(b + 3, 0, ag_forward, layer, 0)
            put(b + 3, 2, ag_forward, layer, 1)
            put(b + 3, 2, ag_finish, layer, 0)
            put(b + 3, 2, ag_finish, layer, 1)
        late = 0 if layer == 0 else 2
        put(b + 1 + late, 1 + late, do_inner, layer)
        put(b + 2 + late, 1, do_value, layer)
        put(b + 3 + late, 1, do_gate, layer)
        put(b + 3 + late, 2, do_conv, layer)
        put(b + 4 + late, 1, do_out, layer)
        after = do_next if layer < layers - 1 else do_result
        put(b + 5 + late, 1, do_stats, layer, 0)
        put(b + 5 + late, 2, after, layer, 0)
        put(b + 6 + late, 0, do_stats, layer, 1)
        put(b + 6 + late, 1, after, layer, 1)

    @pl.when(is_middle)
    def _():
        st_out[...] = jnp.zeros_like(st_out)
        ahead = 2
        for u in range(min(ahead, units)):
            send_own(u)
        x_copy.wait()
        ag_start(0, 1)
        for u in range(units):
            if u + ahead < units:
                send_own(u + ahead)
            for k in range(3):
                event(u, k)
                for step, args in steps.get(3 * u + k, ()):
                    step(*args)

        for u in range(units):
            own_in(u).wait_send()
            forward(u).wait_send()
            across(u, 0, g).wait_send()
            across(u, 1, g).wait_send()
        for layer in range(layers):
            halo_copy(layer).wait_send()
            for h in range(2):
                for i in range(3):
                    ag(layer, h, i).wait_send()
                    stat(layer, h, i).wait_send()
                to_sib(layer, h, 0).wait_send()
                to_sib(layer, h, 1).wait_send()
                to_far(layer, h).wait_send()
        result().wait_send()


def fused(tokens, gate_weight, inner_weight, value_weight, out_weight, taps, norm_gain, norm_bias):
    rows, chan = tokens.shape
    layers = gate_weight.shape[0]
    width = chan * lax.axis_size("tp")
    units = 4 * layers
    dma = pltpu.SemaphoreType.DMA
    hbm = pl.BlockSpec(memory_space=pltpu.HBM)
    vmem = pl.BlockSpec(memory_space=pltpu.VMEM)
    return pl.pallas_call(
        functools.partial(mixer, layers),
        out_shape=jax.ShapeDtypeStruct((rows, chan), BF16),
        in_specs=[hbm] * 5 + [vmem] * 3,
        out_specs=vmem,
        scratch_shapes=[
            pltpu.VMEM((units, width, chan), BF16),
            pltpu.VMEM((layers, 2 * rows, width), BF16),
            pltpu.VMEM((2 * rows, chan), BF16),
            pltpu.VMEM((layers, 2 * rows, chan), BF16),
            pltpu.VMEM((2 * rows, chan), BF16),
            pltpu.VMEM((2 * rows, chan), BF16),
            pltpu.VMEM((2, rows, chan), F32),
            pltpu.VMEM((layers, 16, chan), BF16),
            pltpu.VMEM((rows, chan), BF16),
            pltpu.VMEM((layers, 2, 2, rows, chan), BF16),
            pltpu.VMEM((layers, 2, 2, rows, chan), BF16),
            pltpu.VMEM((layers, 2, rows, chan), BF16),
            pltpu.VMEM((layers, 2, rows, chan), BF16),
            pltpu.VMEM((layers, 2, 8, rows), F32),
            pltpu.VMEM((layers, 2, 3, 8, rows), F32),
            dma((units,)), dma, dma((units,)), dma((units,)),
            dma((units, 2)), dma((units, 2)), dma((units, 2)),
            dma((units, 2)), dma((units, 2)), dma, dma, dma, dma,
            dma((layers,)), dma((layers,)), dma((layers, 2, 3)), dma((layers, 2, 3)),
            dma((layers, 2, 3)), dma((layers, 2, 3)), dma((layers, 2, 3)), dma((layers, 2, 3)),
        ],
        compiler_params=pltpu.CompilerParams(
            collective_id=0, has_side_effects=True, vmem_limit_bytes=58 * 2**20),
    )(tokens, inner_weight, value_weight, gate_weight, out_weight, taps, norm_gain, norm_bias)


def solution(mesh):
    in_specs = (
        P(("grp", "sp"), "tp"),
        P(None, "sp", "tp"),
        P(None, "sp", "tp"),
        P(None, "sp", "tp"),
        P(None, "tp", "sp"),
        P(None, None, "tp"),
        P(None, "tp"),
        P(None, "tp"),
    )
    out_specs = P(("grp", "sp"), "tp")
    routed = (mesh.shape["grp"], mesh.shape["sp"], mesh.shape["tp"]) == (2, 4, 4)
    body = fused if routed else shards
    return jax.shard_map(body, mesh=mesh, in_specs=in_specs, out_specs=out_specs, check_vma=False)
```

```python
import functools

import jax
import jax.numpy as jnp
from jax import lax
from jax.experimental import pallas as pl
from jax.experimental.pallas import tpu as pltpu
from jax.sharding import PartitionSpec as P

MESH = pl.DeviceIdType.MESH
F32 = jnp.float32
BF16 = jnp.bfloat16


def extended(value, sides, width):
    for axis, dim in sides:
        peers, length = (lax.axis_size(axis), value.shape[dim])
        up = [(i, (i + 1) % peers) for i in range(peers - 1)]
        down = [(j, i) for i, j in up]
        last = lax.slice_in_dim(value, length - width, length, axis=dim)
        initial = lax.slice_in_dim(value, 0, width, axis=dim)
        before = lax.ppermute(last, axis, up)
        after = lax.ppermute(initial, axis, down)
        value = jnp.concatenate([before, value, after], axis=dim)
    return value


def shards(tokens, gate_weight, inner_weight, value_weight, out_weight, taps, norm_gain, norm_bias):
    x = tokens
    width = x.shape[1] * lax.axis_size("tp")
    full_gate, full_inner, full_value, full_out = (
        lax.all_gather(gate_weight, "sp", axis=1, tiled=True),
        lax.all_gather(inner_weight, "sp", axis=1, tiled=True),
        lax.all_gather(value_weight, "sp", axis=1, tiled=True),
        lax.all_gather(out_weight, "sp", axis=2, tiled=True),
    )
    for layer in range(gate_weight.shape[0]):
        whole = lax.all_gather(x, "tp", axis=1, tiled=True)
        outer = jnp.dot(whole, full_gate[layer], preferred_element_type=F32).astype(BF16)
        inner = jnp.dot(whole, full_inner[layer], preferred_element_type=F32).astype(BF16)
        values = jnp.dot(whole, full_value[layer], preferred_element_type=F32).astype(BF16)
        product = (inner.astype(F32) * values.astype(F32)).astype(BF16)
        padded = extended(product, (("sp", 0),), 1).astype(F32)
        kernel = taps[layer].astype(F32)
        conv = kernel[0] * padded[:-2] + kernel[1] * padded[1:-1] + kernel[2] * padded[2:]
        gated = (outer.astype(F32) * conv).astype(BF16)
        terms = jnp.dot(gated, full_out[layer], preferred_element_type=F32)
        branch = lax.psum_scatter(
            terms.astype(BF16), "tp", scatter_dimension=1, tiled=True
        ).astype(F32)
        total = 2.0**0.5 * x.astype(F32) + branch
        row_sum, row_square = lax.psum(
            (jnp.sum(total, axis=1), jnp.sum(total * total, axis=1)), "tp"
        )
        mean = (row_sum / width)[:, None]
        spread = (row_square / width)[:, None] - mean * mean
        x = (
            (total - mean) * lax.rsqrt(spread + 1e-05) * norm_gain[layer] + norm_bias[layer]
        ).astype(BF16)
    return x


def mixer(layers, x_hbm, wi, wv, wg, wo, taps, gain, bias, out,
          gbuf, xfull, ibuf, pbuf, obuf, gated, tot, halo, final,
          sib_out, sib_in, far_out, far_in, st_out, st_in,
          s_local, s_x, s_own, s_fwd, s_y, r_z, r_y,
          s_end, r_end, s_tok, r_tok, s_res, r_res,
          s_halo, r_halo, s_ag, r_ag, s_rs, r_rs, s_far, r_far, s_st, r_st):
    g, s, t = lax.axis_index("grp"), lax.axis_index("sp"), lax.axis_index("tp")
    weights = (wi, wv, wg, wo)
    rows, chan = x_hbm.shape
    block = chan
    half = block // 2
    width = xfull.shape[2]
    units = 4 * layers
    last = lax.axis_size("sp") - 1
    sib = t + 1 - 2 * lax.rem(t, 2)
    far = lax.rem(t + 2, 4)
    diag = lax.rem(sib + 2, 4)
    grp_peer = 1 - g
    is_end = jnp.logical_or(s == 0, s == last)
    is_middle = jnp.logical_and(s > 0, s < last)
    mate = s + 1 - 2 * lax.rem(s, 2)
    inner = last - s
    beyond = last - mate

    def column(owner):
        return pl.ds(pl.multiple_of(owner * chan, 128), chan)

    def token_rows(h):
        holder = mate if h == 0 else s
        return pl.ds(pl.multiple_of(lax.rem(holder, 2) * rows, rows), rows)

    step_rows = 128
    per_block = rows // step_rows
    chunks = 2 * per_block

    def inside(c):
        return pl.ds((c % per_block) * step_rows, step_rows)

    def chunk_rows(c):
        holder = mate if c < per_block else s
        start = lax.rem(holder, 2) * rows + (c % per_block) * step_rows
        return pl.ds(pl.multiple_of(start, step_rows), step_rows)

    def local(u):
        layer, m = divmod(u, 4)
        return pltpu.make_async_copy(
            weights[m].at[layer],
            gbuf.at[u, pl.ds(pl.multiple_of(s * block, block), block)],
            s_local.at[u])

    x_copy = pltpu.make_async_copy(x_hbm, xfull.at[0, token_rows(1), column(t)], s_x)
    x_copy.start()
    for u in range(units):
        local(u).start()

    barrier = pltpu.get_barrier_semaphore()

    def hello(dg, ds, dt):
        pl.semaphore_signal(barrier, 1, device_id=(dg, ds, dt), device_id_type=MESH)

    hello(g, mate, t)

    @pl.when(is_middle)
    def _():
        hello(grp_peer, s, t)
        hello(g, inner, t)
        for k in (1, 2, 3):
            hello(g, s, lax.rem(t + k, 4))

    pl.semaphore_wait(barrier, jnp.where(is_middle, 6, 1))

    def remote(src, dst, send, recv, to):
        return pltpu.make_async_remote_copy(
            src_ref=src, dst_ref=dst, send_sem=send, recv_sem=recv,
            device_id=to, device_id_type=MESH)

    def piece(u, src, side):
        return gbuf.at[u, pl.ds(pl.multiple_of(src * block + side * half, half), half)]

    def tokens_in():
        ref = xfull.at[0, token_rows(1), column(t)]
        return remote(ref, ref, s_tok, r_tok, (g, mate, t))

    def end_piece(u, i):
        p = piece(u, s, g if i == 0 else 1 - g)
        return remote(p, p, s_end.at[u, i], r_end.at[u, i], (g, mate, t))

    def result(c):
        return remote(final.at[inside(c)], out.at[inside(c)], s_res.at[c], r_res.at[c], (g, mate, t))

    @pl.when(is_end)
    def _():
        x_copy.wait()
        tokens_in().start()
        order = [(0, 0)]
        for u in range(1, units):
            order += [(u, 0), (u - 1, 1)]
        order += [(units - 1, 1)]
        for u in range(units):
            local(u).wait()
        for n, (u, i) in enumerate(order):
            if n >= 3:
                end_piece(*order[n - 3]).wait_send()
            end_piece(u, i).start()
        for u, i in order[-3:]:
            end_piece(u, i).wait_send()
        tokens_in().wait_send()
        for c in range(per_block):
            result(c).wait_recv()

    def own_in(u):
        p = piece(u, s, g)
        return remote(p, p, s_own.at[u], r_z.at[u, 0], (g, inner, t))

    def forward(u):
        p = piece(u, mate, g)
        return remote(p, p, s_fwd.at[u], r_z.at[u, 1], (g, inner, t))

    def across(u, k, side):
        p = piece(u, inner if k == 0 else beyond, side)
        return remote(p, p, s_y.at[u, k], r_y.at[u, k], (grp_peer, s, t))

    def event(u, k):
        if k == 0:
            p = piece(u, mate, g)
            remote(p, p, s_end.at[u, 0], r_end.at[u, 0], (g, mate, t)).wait_recv()
            forward(u).start()
        else:
            p = piece(u, inner if k == 1 else beyond, g)
            remote(p, p, s_fwd.at[u], r_z.at[u, k - 1], (g, inner, t)).wait_recv()
            across(u, k - 1, g).start()

    def send_own(u):
        local(u).wait()
        own_in(u).start()

    def unit_ready(u):
        p = piece(u, mate, 1 - g)
        remote(p, p, s_end.at[u, 1], r_end.at[u, 1], (g, mate, t)).wait_recv()
        across(u, 0, grp_peer).wait_recv()
        across(u, 1, grp_peer).wait_recv()

    def ag(layer, c, i):
        owner = (t, t, far)[i]
        to = (far, sib, sib)[i]
        ref = xfull.at[layer, chunk_rows(c), column(owner)]
        return remote(ref, ref, s_ag.at[layer, c, i], r_ag.at[layer, c, i], (g, s, to))

    def ag_recv(layer, c, i):
        owner = (far, sib, diag)[i]
        ref = xfull.at[layer, chunk_rows(c), column(owner)]
        remote(ref, ref, s_ag.at[layer, c, i], r_ag.at[layer, c, i], (g, s, sib)).wait_recv()

    def ag_start(layer, c):
        ag(layer, c, 0).start()
        ag(layer, c, 1).start()

    def ag_forward(layer, c):
        ag_recv(layer, c, 0)
        ag(layer, c, 2).start()

    def ag_finish(layer, c):
        ag_recv(layer, c, 1)
        ag_recv(layer, c, 2)

    def adopt():
        ref = xfull.at[0, token_rows(0), column(t)]
        remote(ref, ref, s_tok, r_tok, (g, mate, t)).wait_recv()
        for c in range(per_block):
            ag_start(0, c)

    tile = 256
    tiles = chan // tile

    def project(layer, m, store):
        u = 4 * layer + m
        unit_ready(u)

        @pl.loop(0, 2 * tiles)
        def _(n):
            cols = pl.ds(pl.multiple_of(lax.rem(n, tiles) * tile, tile), tile)
            at = pl.ds(pl.multiple_of((n // tiles) * rows, rows), rows)
            store(at, cols, jnp.dot(xfull[layer, at, :], gbuf[u, :, cols],
                                    preferred_element_type=F32).astype(BF16))

    edge = halo.shape[1]

    def halo_copy(layer):
        edge_row = jnp.where(s < inner, 2 * rows - edge, 0)
        return remote(pbuf.at[layer, pl.ds(pl.multiple_of(edge_row, edge), edge)], halo.at[layer],
                      s_halo.at[layer], r_halo.at[layer], (g, inner, t))

    def do_inner(layer):
        def store(at, cols, value):
            ibuf[at, cols] = value
        project(layer, 0, store)

    def do_value(layer):
        def store(at, cols, value):
            pbuf[layer, at, cols] = (ibuf[at, cols].astype(F32) * value.astype(F32)).astype(BF16)
        project(layer, 1, store)
        halo_copy(layer).start()

    def do_gate(layer):
        def store(at, cols, value):
            obuf[at, cols] = value
        project(layer, 2, store)

    def do_conv(layer):
        halo_copy(layer).wait_recv()

        @pl.loop(0, chan // 128)
        def _(n):
            cols = pl.ds(pl.multiple_of(n * 128, 128), 128)
            p = pbuf[layer, :, cols].astype(F32)
            row = lax.broadcasted_iota(jnp.int32, p.shape, 0)
            met = halo[layer, :, cols].astype(F32)
            first = jnp.where(s > inner, met[edge - 1:edge], 0.0)
            closing = jnp.where(s < inner, met[0:1], 0.0)
            before = jnp.where(row == 0, first, pltpu.roll(p, 1, 0))
            after = jnp.where(row == 2 * rows - 1, closing, pltpu.roll(p, 2 * rows - 1, 0))
            k = taps[layer, :, cols].astype(F32)
            conv = k[0:1] * before + k[1:2] * p + k[2:3] * after
            gated[:, cols] = (obuf[:, cols].astype(F32) * conv).astype(BF16)

    def term(layer, h, owner, store):
        u = 4 * layer + 3
        at = token_rows(h)

        @pl.loop(0, tiles)
        def _(n):
            cols = pl.ds(pl.multiple_of(n * tile, tile), tile)
            w = gbuf[u, pl.ds(pl.multiple_of(owner * block, block), block), cols]
            store(cols, jnp.dot(gated[at, :], w, preferred_element_type=F32).astype(BF16))

    def to_sib(layer, h, i):
        return remote(sib_out.at[layer, h, i], sib_in.at[layer, h, i],
                      s_rs.at[layer, h, i], r_rs.at[layer, h, i], (g, s, sib))

    def to_far(layer, c):
        h = c // per_block
        return remote(far_out.at[layer, h, inside(c)], far_in.at[layer, h, inside(c)],
                      s_far.at[layer, c], r_far.at[layer, c], (g, s, far))

    def do_diag(layer, h):
        def store(cols, value):
            sib_out[layer, h, 0, :, cols] = value
        term(layer, h, diag, store)
        to_sib(layer, h, 0).start()

    def do_sib(layer, h):
        def store(cols, value):
            sib_out[layer, h, 1, :, cols] = value
        term(layer, h, sib, store)
        to_sib(layer, h, 1).start()

    def do_far(layer, h):
        to_sib(layer, h, 0).wait_recv()

        def store(cols, value):
            far_out[layer, h, :, cols] = (
                value.astype(F32) + sib_in[layer, h, 0, :, cols].astype(F32)).astype(BF16)
        term(layer, h, far, store)

    def do_out(layer):
        unit_ready(4 * layer + 3)
        do_diag(layer, 0)
        do_diag(layer, 1)
        do_far(layer, 0)
        to_far(layer, 0).start()
        to_far(layer, 1).start()
        do_sib(layer, 0)
        do_far(layer, 1)
        do_sib(layer, 1)
        do_total(layer, 0)
        do_total(layer, 1)

    def stat(layer, c, i):
        return remote(st_out.at[layer, c], st_in.at[layer, c, i], s_st.at[layer, c, i],
                      r_st.at[layer, c, i], (g, s, (sib, far, diag)[i]))

    def do_total(layer, h):
        to_sib(layer, h, 1).wait_recv()
        at = token_rows(h)

        def store(cols, value):
            mine = pl.ds(pl.multiple_of(t * chan + cols.start, 128), tile)
            tot[h, :, cols] = (2.0**0.5 * xfull[layer, at, mine].astype(F32) + value.astype(F32)
                               + sib_in[layer, h, 1, :, cols].astype(F32))
        term(layer, h, t, store)

    def do_stats(layer, c):
        to_far(layer, c).wait_recv()
        h, at = c // per_block, inside(c)
        total_sum = jnp.zeros((step_rows, 128), F32)
        total_square = jnp.zeros((step_rows, 128), F32)
        for n in range(chan // 128):
            cols = slice(n * 128, n * 128 + 128)
            z = tot[h, at, cols] + far_in[layer, h, at, cols].astype(F32)
            tot[h, at, cols] = z
            total_sum = total_sum + z
            total_square = total_square + z * z
        st_out[layer, c, 0:1, :] = jnp.sum(total_sum.T, axis=0, keepdims=True)
        st_out[layer, c, 1:2, :] = jnp.sum(total_square.T, axis=0, keepdims=True)
        for i in (1, 2, 0):
            stat(layer, c, i).start()

    def do_norm(layer, c):
        for i in range(3):
            stat(layer, c, i).wait_recv()
        h, at = c // per_block, inside(c)
        both = st_out[layer, c] + st_in[layer, c, 0] + st_in[layer, c, 1] + st_in[layer, c, 2]
        mean = both[0:1] / width
        spread = both[1:2] / width - mean * mean
        scale = lax.rsqrt(spread + 1e-05)
        mean = jnp.broadcast_to(mean, (step_rows, step_rows)).T
        scale = jnp.broadcast_to(scale, (step_rows, step_rows)).T
        for n in range(chan // 128):
            cols = slice(n * 128, n * 128 + 128)
            z = (tot[h, at, cols] - mean) * scale * gain[layer:layer + 1, cols] + bias[layer:layer + 1, cols]
            value = z.astype(BF16)
            if layer < layers - 1:
                to = pl.ds(pl.multiple_of(t * chan + n * 128, 128), 128)
                xfull[layer + 1, chunk_rows(c), to] = value
            elif h == 0:
                final[at, cols] = value
            else:
                out[at, cols] = value
        if layer < layers - 1:
            ag_start(layer + 1, c)
        elif h == 0:
            result(c).start()

    def do_chunk(layer, c):
        if c < chunks:
            do_stats(layer, c)
            if c + 2 < chunks:
                to_far(layer, c + 2).start()
        if c > 0:
            do_norm(layer, c - 1)

    steps = {}

    def put(u, k, step, *args):
        at = min(3 * u + k, 3 * units - 1)
        steps.setdefault(at, []).append((step, args))

    put(0, 0, adopt)
    for c in range(per_block):
        put(0, 1, ag_forward, 0, per_block + c)
        put(1, 0, ag_forward, 0, c)
    for c in range(chunks):
        put(1, 1, ag_finish, 0, c)
    for layer in range(layers):
        b = 4 * layer
        if layer > 0:
            for c in range(chunks):
                put(b + 2, 1 + c // per_block, ag_forward, layer, c)
            for c in range(chunks):
                put(b + 3, 0, ag_finish, layer, c)
            put(b + 3, 0, do_inner, layer)
            put(b + 3, 1, do_value, layer)
            put(b + 3, 2, do_gate, layer)
        else:
            put(b + 1, 1, do_inner, layer)
            put(b + 2, 1, do_value, layer)
            put(b + 3, 1, do_gate, layer)
        put(b + 3, 2, do_conv, layer)
        put(b + 4, 1, do_out, layer)
        for c in range(chunks + 1):
            k = 3 * (b + 4) + 2 + c * 5 // chunks
            put(k // 3, k % 3, do_chunk, layer, c)

    @pl.when(is_middle)
    def _():
        st_out[...] = jnp.zeros_like(st_out)
        ahead = 2
        for u in range(min(ahead, units)):
            send_own(u)
        x_copy.wait()
        for c in range(per_block, chunks):
            ag_start(0, c)
        for u in range(units):
            if u + ahead < units:
                send_own(u + ahead)
            for k in range(3):
                event(u, k)
                for step, args in steps.get(3 * u + k, ()):
                    step(*args)

        for u in range(units):
            own_in(u).wait_send()
            forward(u).wait_send()
            across(u, 0, g).wait_send()
            across(u, 1, g).wait_send()
        for layer in range(layers):
            halo_copy(layer).wait_send()
            for c in range(chunks):
                for i in range(3):
                    ag(layer, c, i).wait_send()
                    stat(layer, c, i).wait_send()
                to_far(layer, c).wait_send()
            for h in range(2):
                to_sib(layer, h, 0).wait_send()
                to_sib(layer, h, 1).wait_send()
        for c in range(per_block):
            result(c).wait_send()


def fused(tokens, gate_weight, inner_weight, value_weight, out_weight, taps, norm_gain, norm_bias):
    rows, chan = tokens.shape
    layers = gate_weight.shape[0]
    width = chan * lax.axis_size("tp")
    units = 4 * layers
    chunks = 2 * (rows // 128)
    dma = pltpu.SemaphoreType.DMA
    hbm = pl.BlockSpec(memory_space=pltpu.HBM)
    vmem = pl.BlockSpec(memory_space=pltpu.VMEM)
    return pl.pallas_call(
        functools.partial(mixer, layers),
        out_shape=jax.ShapeDtypeStruct((rows, chan), BF16),
        in_specs=[hbm] * 5 + [vmem] * 3,
        out_specs=vmem,
        scratch_shapes=[
            pltpu.VMEM((units, width, chan), BF16),
            pltpu.VMEM((layers, 2 * rows, width), BF16),
            pltpu.VMEM((2 * rows, chan), BF16),
            pltpu.VMEM((layers, 2 * rows, chan), BF16),
            pltpu.VMEM((2 * rows, chan), BF16),
            pltpu.VMEM((2 * rows, chan), BF16),
            pltpu.VMEM((2, rows, chan), F32),
            pltpu.VMEM((layers, 16, chan), BF16),
            pltpu.VMEM((rows, chan), BF16),
            pltpu.VMEM((layers, 2, 2, rows, chan), BF16),
            pltpu.VMEM((layers, 2, 2, rows, chan), BF16),
            pltpu.VMEM((layers, 2, rows, chan), BF16),
            pltpu.VMEM((layers, 2, rows, chan), BF16),
            pltpu.VMEM((layers, chunks, 8, 128), F32),
            pltpu.VMEM((layers, chunks, 3, 8, 128), F32),
            dma((units,)), dma, dma((units,)), dma((units,)),
            dma((units, 2)), dma((units, 2)), dma((units, 2)),
            dma((units, 2)), dma((units, 2)), dma, dma, dma((chunks,)), dma((chunks,)),
            dma((layers,)), dma((layers,)), dma((layers, chunks, 3)), dma((layers, chunks, 3)),
            dma((layers, 2, 2)), dma((layers, 2, 2)), dma((layers, chunks)), dma((layers, chunks)),
            dma((layers, chunks, 3)), dma((layers, chunks, 3)),
        ],
        compiler_params=pltpu.CompilerParams(
            collective_id=0, has_side_effects=True, vmem_limit_bytes=58 * 2**20),
    )(tokens, inner_weight, value_weight, gate_weight, out_weight, taps, norm_gain, norm_bias)


def solution(mesh):
    in_specs = (
        P(("grp", "sp"), "tp"),
        P(None, "sp", "tp"),
        P(None, "sp", "tp"),
        P(None, "sp", "tp"),
        P(None, "tp", "sp"),
        P(None, None, "tp"),
        P(None, "tp"),
        P(None, "tp"),
    )
    out_specs = P(("grp", "sp"), "tp")
    routed = (mesh.shape["grp"], mesh.shape["sp"], mesh.shape["tp"]) == (2, 4, 4)
    body = fused if routed else shards
    return jax.shard_map(body, mesh=mesh, in_specs=in_specs, out_specs=out_specs, check_vma=False)
```

```python
import functools

import jax
import jax.numpy as jnp
from jax import lax
from jax.experimental import pallas as pl
from jax.experimental.pallas import tpu as pltpu
from jax.sharding import PartitionSpec as P

MESH = pl.DeviceIdType.MESH
F32 = jnp.float32
BF16 = jnp.bfloat16


def extended(value, sides, width):
    for axis, dim in sides:
        peers, length = (lax.axis_size(axis), value.shape[dim])
        up = [(i, (i + 1) % peers) for i in range(peers - 1)]
        down = [(j, i) for i, j in up]
        last = lax.slice_in_dim(value, length - width, length, axis=dim)
        initial = lax.slice_in_dim(value, 0, width, axis=dim)
        before = lax.ppermute(last, axis, up)
        after = lax.ppermute(initial, axis, down)
        value = jnp.concatenate([before, value, after], axis=dim)
    return value


def shards(tokens, gate_weight, inner_weight, value_weight, out_weight, taps, norm_gain, norm_bias):
    x = tokens
    width = x.shape[1] * lax.axis_size("tp")
    full_gate, full_inner, full_value, full_out = (
        lax.all_gather(gate_weight, "sp", axis=1, tiled=True),
        lax.all_gather(inner_weight, "sp", axis=1, tiled=True),
        lax.all_gather(value_weight, "sp", axis=1, tiled=True),
        lax.all_gather(out_weight, "sp", axis=2, tiled=True),
    )
    for layer in range(gate_weight.shape[0]):
        whole = lax.all_gather(x, "tp", axis=1, tiled=True)
        outer = jnp.dot(whole, full_gate[layer], preferred_element_type=F32).astype(BF16)
        inner = jnp.dot(whole, full_inner[layer], preferred_element_type=F32).astype(BF16)
        values = jnp.dot(whole, full_value[layer], preferred_element_type=F32).astype(BF16)
        product = (inner.astype(F32) * values.astype(F32)).astype(BF16)
        padded = extended(product, (("sp", 0),), 1).astype(F32)
        kernel = taps[layer].astype(F32)
        conv = kernel[0] * padded[:-2] + kernel[1] * padded[1:-1] + kernel[2] * padded[2:]
        gated = (outer.astype(F32) * conv).astype(BF16)
        terms = jnp.dot(gated, full_out[layer], preferred_element_type=F32)
        branch = lax.psum_scatter(
            terms.astype(BF16), "tp", scatter_dimension=1, tiled=True
        ).astype(F32)
        total = 2.0**0.5 * x.astype(F32) + branch
        row_sum, row_square = lax.psum(
            (jnp.sum(total, axis=1), jnp.sum(total * total, axis=1)), "tp"
        )
        mean = (row_sum / width)[:, None]
        spread = (row_square / width)[:, None] - mean * mean
        x = (
            (total - mean) * lax.rsqrt(spread + 1e-05) * norm_gain[layer] + norm_bias[layer]
        ).astype(BF16)
    return x


def mixer(layers, x_hbm, wi, wv, wg, wo, taps, gain, bias, out,
          gbuf, xfull, ibuf, pbuf, obuf, gated, tot, halo, final,
          sib_out, sib_in, far_out, far_in, st_out, st_in,
          s_local, s_x, s_own, s_fwd, s_y, r_z, r_y,
          s_end, r_end, s_tok, r_tok, s_res, r_res,
          s_halo, r_halo, s_ag, r_ag, s_rs, r_rs, s_far, r_far, s_st, r_st):
    g, s, t = lax.axis_index("grp"), lax.axis_index("sp"), lax.axis_index("tp")
    weights = (wi, wv, wg, wo)
    rows, chan = x_hbm.shape
    block = chan
    half = block // 2
    width = xfull.shape[2]
    units = 4 * layers
    last = lax.axis_size("sp") - 1
    sib = t + 1 - 2 * lax.rem(t, 2)
    far = lax.rem(t + 2, 4)
    diag = lax.rem(sib + 2, 4)
    grp_peer = 1 - g
    is_end = jnp.logical_or(s == 0, s == last)
    is_middle = jnp.logical_and(s > 0, s < last)
    mate = s + 1 - 2 * lax.rem(s, 2)
    inner = last - s
    beyond = last - mate

    def column(owner):
        return pl.ds(pl.multiple_of(owner * chan, 128), chan)

    def token_rows(h):
        holder = mate if h == 0 else s
        return pl.ds(pl.multiple_of(lax.rem(holder, 2) * rows, rows), rows)

    step_rows = 128
    per_block = rows // step_rows
    chunks = 2 * per_block

    def inside(c):
        return pl.ds((c % per_block) * step_rows, step_rows)

    def chunk_rows(c):
        holder = mate if c < per_block else s
        start = lax.rem(holder, 2) * rows + (c % per_block) * step_rows
        return pl.ds(pl.multiple_of(start, step_rows), step_rows)

    def local(u):
        layer, m = divmod(u, 4)
        return pltpu.make_async_copy(
            weights[m].at[layer],
            gbuf.at[u, pl.ds(pl.multiple_of(s * block, block), block)],
            s_local.at[u])

    x_copy = pltpu.make_async_copy(x_hbm, xfull.at[0, token_rows(1), column(t)], s_x)
    x_copy.start()
    for u in range(units):
        local(u).start()

    barrier = pltpu.get_barrier_semaphore()

    def hello(dg, ds, dt):
        pl.semaphore_signal(barrier, 1, device_id=(dg, ds, dt), device_id_type=MESH)

    hello(g, mate, t)

    @pl.when(is_middle)
    def _():
        hello(grp_peer, s, t)
        hello(g, inner, t)
        for k in (1, 2, 3):
            hello(g, s, lax.rem(t + k, 4))

    pl.semaphore_wait(barrier, jnp.where(is_middle, 6, 1))

    def remote(src, dst, send, recv, to):
        return pltpu.make_async_remote_copy(
            src_ref=src, dst_ref=dst, send_sem=send, recv_sem=recv,
            device_id=to, device_id_type=MESH)

    def piece(u, src, side):
        return gbuf.at[u, pl.ds(pl.multiple_of(src * block + side * half, half), half)]

    def tokens_in():
        ref = xfull.at[0, token_rows(1), column(t)]
        return remote(ref, ref, s_tok, r_tok, (g, mate, t))

    def end_piece(u, i):
        p = piece(u, s, g if i == 0 else 1 - g)
        return remote(p, p, s_end.at[u, i], r_end.at[u, i], (g, mate, t))

    def result(c):
        return remote(final.at[inside(c)], out.at[inside(c)], s_res.at[c], r_res.at[c], (g, mate, t))

    @pl.when(is_end)
    def _():
        local(0).wait()
        end_piece(0, 0).start()
        x_copy.wait()
        tokens_in().start()
        order = [(0, 0)]
        for u in range(1, units):
            order += [(u, 0), (u - 1, 1)]
        order += [(units - 1, 1)]
        for u in range(1, units):
            local(u).wait()
        for n, (u, i) in enumerate(order):
            if n >= 3:
                end_piece(*order[n - 3]).wait_send()
            if n > 0:
                end_piece(u, i).start()
        for u, i in order[-3:]:
            end_piece(u, i).wait_send()
        tokens_in().wait_send()
        for c in range(per_block):
            result(c).wait_recv()

    def own_in(u):
        p = piece(u, s, g)
        return remote(p, p, s_own.at[u], r_z.at[u, 0], (g, inner, t))

    def forward(u):
        p = piece(u, mate, g)
        return remote(p, p, s_fwd.at[u], r_z.at[u, 1], (g, inner, t))

    def across(u, k, side):
        p = piece(u, inner if k == 0 else beyond, side)
        return remote(p, p, s_y.at[u, k], r_y.at[u, k], (grp_peer, s, t))

    def event(u, k):
        if k == 0:
            p = piece(u, mate, g)
            remote(p, p, s_end.at[u, 0], r_end.at[u, 0], (g, mate, t)).wait_recv()
            forward(u).start()
        else:
            p = piece(u, inner if k == 1 else beyond, g)
            remote(p, p, s_fwd.at[u], r_z.at[u, k - 1], (g, inner, t)).wait_recv()
            across(u, k - 1, g).start()

    def send_own(u):
        local(u).wait()
        own_in(u).start()

    def unit_ready(u):
        p = piece(u, mate, 1 - g)
        remote(p, p, s_end.at[u, 1], r_end.at[u, 1], (g, mate, t)).wait_recv()
        across(u, 0, grp_peer).wait_recv()
        across(u, 1, grp_peer).wait_recv()

    def ag(layer, c, i):
        owner = (t, t, far)[i]
        to = (far, sib, sib)[i]
        ref = xfull.at[layer, chunk_rows(c), column(owner)]
        return remote(ref, ref, s_ag.at[layer, c, i], r_ag.at[layer, c, i], (g, s, to))

    def ag_recv(layer, c, i):
        owner = (far, sib, diag)[i]
        ref = xfull.at[layer, chunk_rows(c), column(owner)]
        remote(ref, ref, s_ag.at[layer, c, i], r_ag.at[layer, c, i], (g, s, sib)).wait_recv()

    def ag_start(layer, c):
        ag(layer, c, 0).start()
        ag(layer, c, 1).start()

    def ag_forward(layer, c):
        ag_recv(layer, c, 0)
        ag(layer, c, 2).start()

    def ag_finish(layer, c):
        ag_recv(layer, c, 1)
        ag_recv(layer, c, 2)

    def adopt():
        ref = xfull.at[0, token_rows(0), column(t)]
        remote(ref, ref, s_tok, r_tok, (g, mate, t)).wait_recv()
        for c in range(per_block):
            ag_start(0, c)

    tile = 256
    tiles = chan // tile

    def project(layer, m, store):
        u = 4 * layer + m
        unit_ready(u)

        @pl.loop(0, 2 * tiles)
        def _(n):
            cols = pl.ds(pl.multiple_of(lax.rem(n, tiles) * tile, tile), tile)
            at = pl.ds(pl.multiple_of((n // tiles) * rows, rows), rows)
            store(at, cols, jnp.dot(xfull[layer, at, :], gbuf[u, :, cols],
                                    preferred_element_type=F32).astype(BF16))

    edge = halo.shape[1]

    def halo_copy(layer):
        edge_row = jnp.where(s < inner, 2 * rows - edge, 0)
        return remote(pbuf.at[layer, pl.ds(pl.multiple_of(edge_row, edge), edge)], halo.at[layer],
                      s_halo.at[layer], r_halo.at[layer], (g, inner, t))

    def do_inner(layer):
        def store(at, cols, value):
            ibuf[at, cols] = value
        project(layer, 0, store)

    def do_value(layer):
        def store(at, cols, value):
            pbuf[layer, at, cols] = (ibuf[at, cols].astype(F32) * value.astype(F32)).astype(BF16)
        project(layer, 1, store)
        halo_copy(layer).start()

    def do_gate(layer):
        def store(at, cols, value):
            obuf[at, cols] = value
        project(layer, 2, store)

    def do_conv(layer):
        halo_copy(layer).wait_recv()

        @pl.loop(0, chan // 128)
        def _(n):
            cols = pl.ds(pl.multiple_of(n * 128, 128), 128)
            p = pbuf[layer, :, cols].astype(F32)
            row = lax.broadcasted_iota(jnp.int32, p.shape, 0)
            met = halo[layer, :, cols].astype(F32)
            first = jnp.where(s > inner, met[edge - 1:edge], 0.0)
            closing = jnp.where(s < inner, met[0:1], 0.0)
            before = jnp.where(row == 0, first, pltpu.roll(p, 1, 0))
            after = jnp.where(row == 2 * rows - 1, closing, pltpu.roll(p, 2 * rows - 1, 0))
            k = taps[layer, :, cols].astype(F32)
            conv = k[0:1] * before + k[1:2] * p + k[2:3] * after
            gated[:, cols] = (obuf[:, cols].astype(F32) * conv).astype(BF16)

    def term(layer, h, owner, store):
        u = 4 * layer + 3
        at = token_rows(h)

        @pl.loop(0, tiles)
        def _(n):
            cols = pl.ds(pl.multiple_of(n * tile, tile), tile)
            w = gbuf[u, pl.ds(pl.multiple_of(owner * block, block), block), cols]
            store(cols, jnp.dot(gated[at, :], w, preferred_element_type=F32).astype(BF16))

    def to_sib(layer, h, i):
        return remote(sib_out.at[layer, h, i], sib_in.at[layer, h, i],
                      s_rs.at[layer, h, i], r_rs.at[layer, h, i], (g, s, sib))

    def to_far(layer, c):
        h = c // per_block
        return remote(far_out.at[layer, h, inside(c)], far_in.at[layer, h, inside(c)],
                      s_far.at[layer, c], r_far.at[layer, c], (g, s, far))

    def do_diag(layer, h):
        def store(cols, value):
            sib_out[layer, h, 0, :, cols] = value
        term(layer, h, diag, store)
        to_sib(layer, h, 0).start()

    def do_sib(layer, h):
        def store(cols, value):
            sib_out[layer, h, 1, :, cols] = value
        term(layer, h, sib, store)
        to_sib(layer, h, 1).start()

    def do_far(layer, h):
        to_sib(layer, h, 0).wait_recv()

        def store(cols, value):
            far_out[layer, h, :, cols] = (
                value.astype(F32) + sib_in[layer, h, 0, :, cols].astype(F32)).astype(BF16)
        term(layer, h, far, store)

    def do_out(layer):
        unit_ready(4 * layer + 3)
        do_diag(layer, 0)
        do_diag(layer, 1)
        do_far(layer, 0)
        to_far(layer, 0).start()
        to_far(layer, 1).start()
        do_sib(layer, 0)
        do_far(layer, 1)
        do_sib(layer, 1)
        do_total(layer, 0)
        do_total(layer, 1)

    def stat(layer, c, i):
        return remote(st_out.at[layer, c], st_in.at[layer, c, i], s_st.at[layer, c, i],
                      r_st.at[layer, c, i], (g, s, (sib, far, diag)[i]))

    def do_total(layer, h):
        to_sib(layer, h, 1).wait_recv()
        at = token_rows(h)

        def store(cols, value):
            mine = pl.ds(pl.multiple_of(t * chan + cols.start, 128), tile)
            tot[h, :, cols] = (2.0**0.5 * xfull[layer, at, mine].astype(F32) + value.astype(F32)
                               + sib_in[layer, h, 1, :, cols].astype(F32))
        term(layer, h, t, store)

    def do_stats(layer, c):
        to_far(layer, c).wait_recv()
        h, at = c // per_block, inside(c)
        total_sum = jnp.zeros((step_rows, 128), F32)
        total_square = jnp.zeros((step_rows, 128), F32)
        for n in range(chan // 128):
            cols = slice(n * 128, n * 128 + 128)
            z = tot[h, at, cols] + far_in[layer, h, at, cols].astype(F32)
            tot[h, at, cols] = z
            total_sum = total_sum + z
            total_square = total_square + z * z
        st_out[layer, c, 0:1, :] = jnp.sum(total_sum.T, axis=0, keepdims=True)
        st_out[layer, c, 1:2, :] = jnp.sum(total_square.T, axis=0, keepdims=True)
        for i in (1, 2, 0):
            stat(layer, c, i).start()

    def do_norm(layer, c):
        for i in range(3):
            stat(layer, c, i).wait_recv()
        h, at = c // per_block, inside(c)
        both = st_out[layer, c] + st_in[layer, c, 0] + st_in[layer, c, 1] + st_in[layer, c, 2]
        mean = both[0:1] / width
        spread = both[1:2] / width - mean * mean
        scale = lax.rsqrt(spread + 1e-05)
        mean = jnp.broadcast_to(mean, (step_rows, step_rows)).T
        scale = jnp.broadcast_to(scale, (step_rows, step_rows)).T
        for n in range(chan // 128):
            cols = slice(n * 128, n * 128 + 128)
            z = (tot[h, at, cols] - mean) * scale * gain[layer:layer + 1, cols] + bias[layer:layer + 1, cols]
            value = z.astype(BF16)
            if layer < layers - 1:
                to = pl.ds(pl.multiple_of(t * chan + n * 128, 128), 128)
                xfull[layer + 1, chunk_rows(c), to] = value
            elif h == 0:
                final[at, cols] = value
            else:
                out[at, cols] = value
        if layer < layers - 1:
            ag_start(layer + 1, c)
        elif h == 0:
            result(c).start()

    def do_chunk(layer, c):
        if c < chunks:
            do_stats(layer, c)
            if c + 2 < chunks:
                to_far(layer, c + 2).start()
        if c > 0:
            do_norm(layer, c - 1)

    steps = {}

    def put(u, k, step, *args):
        at = min(3 * u + k, 3 * units - 1)
        steps.setdefault(at, []).append((step, args))

    put(0, 0, adopt)
    for c in range(per_block):
        put(0, 1, ag_forward, 0, per_block + c)
        put(1, 0, ag_forward, 0, c)
    for c in range(chunks):
        put(1, 1, ag_finish, 0, c)
    for layer in range(layers):
        b = 4 * layer
        if layer > 0:
            for c in range(chunks):
                put(b + 2, 1 + c // per_block, ag_forward, layer, c)
            for c in range(chunks):
                put(b + 3, 0, ag_finish, layer, c)
            put(b + 3, 0, do_inner, layer)
            put(b + 3, 1, do_value, layer)
            put(b + 3, 2, do_gate, layer)
        else:
            put(b + 1, 1, do_inner, layer)
            put(b + 2, 1, do_value, layer)
            put(b + 3, 1, do_gate, layer)
        put(b + 3, 2, do_conv, layer)
        put(b + 4, 1, do_out, layer)
        for c in range(chunks + 1):
            k = 3 * (b + 4) + 2 + c * 5 // chunks
            put(k // 3, k % 3, do_chunk, layer, c)

    @pl.when(is_middle)
    def _():
        st_out[...] = jnp.zeros_like(st_out)
        ahead = 2
        for u in range(min(ahead, units)):
            send_own(u)
        x_copy.wait()
        for c in range(per_block, chunks):
            ag_start(0, c)
        for u in range(units):
            if u + ahead < units:
                send_own(u + ahead)
            for k in range(3):
                event(u, k)
                for step, args in steps.get(3 * u + k, ()):
                    step(*args)

        for u in range(units):
            own_in(u).wait_send()
            forward(u).wait_send()
            across(u, 0, g).wait_send()
            across(u, 1, g).wait_send()
        for layer in range(layers):
            halo_copy(layer).wait_send()
            for c in range(chunks):
                for i in range(3):
                    ag(layer, c, i).wait_send()
                    stat(layer, c, i).wait_send()
                to_far(layer, c).wait_send()
            for h in range(2):
                to_sib(layer, h, 0).wait_send()
                to_sib(layer, h, 1).wait_send()
        for c in range(per_block):
            result(c).wait_send()


def fused(tokens, gate_weight, inner_weight, value_weight, out_weight, taps, norm_gain, norm_bias):
    rows, chan = tokens.shape
    layers = gate_weight.shape[0]
    width = chan * lax.axis_size("tp")
    units = 4 * layers
    chunks = 2 * (rows // 128)
    dma = pltpu.SemaphoreType.DMA
    hbm = pl.BlockSpec(memory_space=pltpu.HBM)
    vmem = pl.BlockSpec(memory_space=pltpu.VMEM)
    return pl.pallas_call(
        functools.partial(mixer, layers),
        out_shape=jax.ShapeDtypeStruct((rows, chan), BF16),
        in_specs=[hbm] * 5 + [vmem] * 3,
        out_specs=vmem,
        scratch_shapes=[
            pltpu.VMEM((units, width, chan), BF16),
            pltpu.VMEM((layers, 2 * rows, width), BF16),
            pltpu.VMEM((2 * rows, chan), BF16),
            pltpu.VMEM((layers, 2 * rows, chan), BF16),
            pltpu.VMEM((2 * rows, chan), BF16),
            pltpu.VMEM((2 * rows, chan), BF16),
            pltpu.VMEM((2, rows, chan), F32),
            pltpu.VMEM((layers, 16, chan), BF16),
            pltpu.VMEM((rows, chan), BF16),
            pltpu.VMEM((layers, 2, 2, rows, chan), BF16),
            pltpu.VMEM((layers, 2, 2, rows, chan), BF16),
            pltpu.VMEM((layers, 2, rows, chan), BF16),
            pltpu.VMEM((layers, 2, rows, chan), BF16),
            pltpu.VMEM((layers, chunks, 8, 128), F32),
            pltpu.VMEM((layers, chunks, 3, 8, 128), F32),
            dma((units,)), dma, dma((units,)), dma((units,)),
            dma((units, 2)), dma((units, 2)), dma((units, 2)),
            dma((units, 2)), dma((units, 2)), dma, dma, dma((chunks,)), dma((chunks,)),
            dma((layers,)), dma((layers,)), dma((layers, chunks, 3)), dma((layers, chunks, 3)),
            dma((layers, 2, 2)), dma((layers, 2, 2)), dma((layers, chunks)), dma((layers, chunks)),
            dma((layers, chunks, 3)), dma((layers, chunks, 3)),
        ],
        compiler_params=pltpu.CompilerParams(
            collective_id=0, has_side_effects=True, vmem_limit_bytes=58 * 2**20),
    )(tokens, inner_weight, value_weight, gate_weight, out_weight, taps, norm_gain, norm_bias)


def solution(mesh):
    in_specs = (
        P(("grp", "sp"), "tp"),
        P(None, "sp", "tp"),
        P(None, "sp", "tp"),
        P(None, "sp", "tp"),
        P(None, "tp", "sp"),
        P(None, None, "tp"),
        P(None, "tp"),
        P(None, "tp"),
    )
    out_specs = P(("grp", "sp"), "tp")
    routed = (mesh.shape["grp"], mesh.shape["sp"], mesh.shape["tp"]) == (2, 4, 4)
    body = fused if routed else shards
    return jax.shard_map(body, mesh=mesh, in_specs=in_specs, out_specs=out_specs, check_vma=False)
```
